32 devices in a mesh: sp: 16 (over z, y, x), tp: 2 (over core).
Axes of the slice: x: 2, y: 2, z: 4, core: 2. Of those that a mesh axis runs over, the one named last changes fastest.
Arguments:
- resid: bfloat16 [6144, 2048], P('sp', 'tp'), may hold values from -40 to 40
- query_one: bfloat16 [6144, 1024], P('sp', 'tp'), may hold values from -64 to 64
- key_one: bfloat16 [6144, 1024], P('sp', 'tp'), may hold values from -64 to 64
- query_two: bfloat16 [6144, 1024], P('sp', 'tp'), may hold values from -64 to 64
- key_two: bfloat16 [6144, 1024], P('sp', 'tp'), may hold values from -64 to 64
- values: bfloat16 [6144, 2048], P('sp', 'tp'), may hold values from -6 to 6
- mix_lambda: float32 [8], P('tp'), may hold values from 0.3 to 0.8
- segments: int32 [6144], P('sp'), may hold values from 0 to 7, never falling along the last dimension, each value on 1 to 1536 neighbouring positions
- head_gain: float32 [256], replicated, may hold values from 0.1 to 1.9
- out_weight: bfloat16 [2048, 2048], P(None, 'tp'), may hold values from -0.125 to 0.125
- mixer_gain: float32 [2048], P('tp'), may hold values from 0.1 to 1.9
- gate_weight: bfloat16 [2048, 6144], P('sp', 'tp'), may hold values from -0.125 to 0.125
- up_weight: bfloat16 [2048, 6144], P('sp', 'tp'), may hold values from -0.125 to 0.125
- down_weight: bfloat16 [6144, 2048], P('tp', 'sp'), may hold values from -0.078125 to 0.078125
Outputs:
- layer_out: bfloat16 [6144, 2048], P('sp', 'tp')
The draws below stay inside these ranges and needn't reach their ends.
Inputs may be any that keep to these rules, and one draw needn't show every extreme that they name: `segments`: numbers never fall along the sequence; each document has at most 1536 positions and one has exactly that many.
All inputs are finite; a program needn't handle non-finite values.
Results may differ from the reference program's by a relative error of at most 0.012.
Values may be sent and summed in bfloat16 or wider, within the bound.
A program may use at most 128 MiB of HBM per device.

```python
import math
import jax
import jax.numpy as jnp
import numpy as np
from jax import lax

D = 2048
HEADS = 8
HD = 128
VD = 256
FF = 6144
TOK_DEV = 384
REACH = 4
DOC_MOST = 1536
TOKENS = 6144
DOCS = 8
N_SP = 16
N_TP = 2


def draw_resid(key, part):
    base = jax.random.normal(jax.random.fold_in(key, 11), (TOKENS, D), jnp.float32)
    column = jnp.exp(1.6 * jnp.arange(D, dtype=jnp.float32) / D)
    result = base * column / 2.0
    return jnp.clip(result, -40.0, 40.0).astype(jnp.bfloat16)


def drawn_pair(key, which):
    pair_key = jax.random.fold_in(key, 100 + which)
    width = HEADS * HD
    query = 1.3 * jax.random.normal(jax.random.fold_in(pair_key, 1), (TOKENS, width), jnp.float32)
    keys = 1.3 * jax.random.normal(jax.random.fold_in(pair_key, 2), (TOKENS, width), jnp.float32)
    return (jnp.clip(query, -64.0, 64.0), jnp.clip(keys, -64.0, 64.0))


def draw_query_one(key, part):
    return drawn_pair(key, 1)[0].astype(jnp.bfloat16)


def draw_key_one(key, part):
    return drawn_pair(key, 1)[1].astype(jnp.bfloat16)


def draw_query_two(key, part):
    return drawn_pair(key, 2)[0].astype(jnp.bfloat16)


def draw_key_two(key, part):
    return drawn_pair(key, 2)[1].astype(jnp.bfloat16)


def level_of(own_key, dims, cuts, smallest, largest):
    factor_of = 1.0
    for dim, shards_of in cuts:
        draws = jax.random.uniform(jax.random.fold_in(jax.random.fold_in(own_key, 6), dim), (shards_of,), jnp.float32, smallest / len(cuts), largest / len(cuts))
        factor_of = factor_of * jnp.repeat(jnp.exp(draws), dims[dim] // shards_of).reshape((-1,) + (1,) * (len(dims) - 1 - dim))
    return factor_of


def length_profile(number_of, total, bound, lean):
    weights = [(1 << 20) // math.isqrt(grade ** lean) + 1 for grade in range(2, number_of + 1)]
    rest, counts = total - bound - (number_of - 1), [1] * (number_of - 1)
    while rest > 0:
        movable = [i for i in range(number_of - 1) if counts[i] < bound]
        pool, left = sum([weights[i] for i in movable]), rest
        for i in movable:
            addition = min(bound - counts[i], max(1, left * weights[i] // pool), rest)
            counts[i] = counts[i] + addition
            rest = rest - addition
    return np.array([bound] + counts)


def uneven_parts(rng, count, total, limit, slope):
    if count == 2:
        one = jax.random.randint(rng, (), max(1, total - limit), min(limit, total - 1) + 1)
        return jnp.stack([one, total - one])
    sizes = jnp.asarray(length_profile(count, total, limit, slope), jnp.int32)
    pairs = (count - 1) // 2
    giver, receiver = sizes[1:1 + 2 * pairs:2], sizes[2:2 + 2 * pairs:2]
    slack = jnp.minimum(giver - 1, limit - receiver)
    moved = jax.random.randint(jax.random.fold_in(rng, 1), (pairs,), 0, 1 << 20) % (slack + 1)
    sizes = sizes.at[1:1 + 2 * pairs:2].set(giver - moved).at[2:2 + 2 * pairs:2].set(receiver + moved)
    return sizes[jax.random.permutation(jax.random.fold_in(rng, 2), count)]


def normal_values(stream_key, dims, scale, reach, split=(), kind=jnp.bfloat16):
    values = jax.random.normal(stream_key, dims, jnp.float32) * scale
    if len(split) > 0:
        values = level_of(stream_key, dims, split, -0.22, 0.18) * values
    return jnp.clip(values, min=-reach, max=reach).astype(kind)


def setup_inputs(seed: int = 0) -> dict:
    arg_keys = jax.random.split(jax.random.key(seed), 15)
    resid = draw_resid(jax.random.fold_in(arg_keys[14], 71), 0)
    query_one = draw_query_one(jax.random.fold_in(arg_keys[14], 71), 0)
    key_one = draw_key_one(jax.random.fold_in(arg_keys[14], 71), 0)
    query_two = draw_query_two(jax.random.fold_in(arg_keys[14], 71), 0)
    key_two = draw_key_two(jax.random.fold_in(arg_keys[14], 71), 0)
    values = normal_values(arg_keys[5], (TOKENS, HEADS * VD), 1.0, 6.0, ((0, 16), (1, 2)))
    mix_lambda = jnp.clip(0.3 + 0.5 * jax.random.uniform(arg_keys[6], (HEADS,), jnp.float32) ** level_of(arg_keys[6], (HEADS,), ((0, 2),), -0.2, 0.2), 0.3, 0.8)
    segments = jnp.searchsorted(jnp.cumsum(uneven_parts(arg_keys[7], DOCS, TOKENS, DOC_MOST, 0)), jnp.arange(TOKENS), side="right").astype(jnp.int32)
    head_gain = jnp.clip(1.0 + 0.18 * jax.random.normal(arg_keys[8], (VD,), jnp.float32), 0.1, 1.9)
    out_weight = normal_values(arg_keys[9], (HEADS * VD, D), (HEADS * VD) ** -0.5, 0.125, ((1, 2),))
    mixer_gain = jnp.clip(1.0 + 0.18 * jax.random.normal(arg_keys[10], (D,), jnp.float32), 0.1, 1.9)
    gate_weight = normal_values(arg_keys[11], (D, FF), D ** -0.5, 0.125, ((0, 16), (1, 2)))
    up_weight = normal_values(arg_keys[12], (D, FF), D ** -0.5, 0.125, ((0, 16), (1, 2)))
    down_weight = normal_values(arg_keys[13], (FF, D), FF ** -0.5, 0.078125, ((0, 2), (1, 16)))
    return {"resid": resid, "query_one": query_one, "key_one": key_one, "query_two": query_two, "key_two": key_two, "values": values, "mix_lambda": mix_lambda, "segments": segments, "head_gain": head_gain, "out_weight": out_weight, "mixer_gain": mixer_gain, "gate_weight": gate_weight, "up_weight": up_weight, "down_weight": down_weight}


def reference(resid, query_one, key_one, query_two, key_two, values, mix_lambda, segments, head_gain, out_weight, mixer_gain, gate_weight, up_weight, down_weight):
    rows = TOK_DEV
    span = REACH * TOK_DEV

    def padded(array):
        return jnp.concatenate([jnp.zeros((span,) + array.shape[1:], array.dtype), array], 0)
    key_first = padded(key_one)
    key_second = padded(key_two)
    value_pad = padded(values)
    seg_pad = jnp.concatenate([jnp.full((span,), -1, jnp.int32), segments.astype(jnp.int32)], 0)

    def block(index):
        start = (index * rows).astype(jnp.int32)
        width = span + rows
        q_first = lax.dynamic_slice_in_dim(query_one, start, rows, 0).reshape(rows, HEADS, HD).astype(jnp.float32)
        q_second = lax.dynamic_slice_in_dim(query_two, start, rows, 0).reshape(rows, HEADS, HD).astype(jnp.float32)
        k_first = lax.dynamic_slice_in_dim(key_first, start, width, 0).reshape(width, HEADS, HD).astype(jnp.float32)
        k_second = lax.dynamic_slice_in_dim(key_second, start, width, 0).reshape(width, HEADS, HD).astype(jnp.float32)
        vals = lax.dynamic_slice_in_dim(value_pad, start, width, 0).reshape(width, HEADS, VD).astype(jnp.float32)
        seg_query = lax.dynamic_slice_in_dim(segments.astype(jnp.int32), start, rows, 0)
        seg_key = lax.dynamic_slice_in_dim(seg_pad, start, width, 0)
        q_pos = start + jnp.arange(rows, dtype=jnp.int32)
        k_pos = start - span + jnp.arange(width, dtype=jnp.int32)
        allowed = (seg_key[None, :] == seg_query[:, None]) & (k_pos[None, :] <= q_pos[:, None]) & (k_pos[None, :] >= 0)

        def weights(query, keys):
            score = jnp.einsum('qhd,khd->hqk', query, keys) * HD ** (-0.5)
            score = jnp.where(allowed[None], score, -jnp.inf)
            score = score - lax.optimization_barrier(jnp.max(score, axis=-1, keepdims=True))
            expo = jnp.exp(score)
            return (expo / lax.optimization_barrier(jnp.sum(expo, axis=-1, keepdims=True))).astype(jnp.bfloat16)
        probs_first = weights(q_first, k_first).astype(jnp.float32)
        probs_second = weights(q_second, k_second).astype(jnp.float32)
        out_first = jnp.einsum('hqk,khe->qhe', probs_first, vals)
        out_second = jnp.einsum('hqk,khe->qhe', probs_second, vals)
        head_out = out_first - mix_lambda[None, :, None] * out_second
        meansq = lax.optimization_barrier(jnp.mean(head_out * head_out, axis=-1, keepdims=True))
        normal = head_out * lax.rsqrt(meansq + 1e-05) * head_gain
        return normal.reshape(rows, HEADS * VD).astype(jnp.bfloat16)
    attn_rows = lax.map(block, jnp.arange(N_SP, dtype=jnp.int32)).reshape(TOKENS, HEADS * VD)
    mid = (resid.astype(jnp.float32) + jnp.dot(attn_rows, out_weight, preferred_element_type=jnp.float32)).astype(jnp.bfloat16)
    midf = mid.astype(jnp.float32)
    meansq = lax.optimization_barrier(jnp.mean(midf * midf, axis=-1, keepdims=True))
    normed = (midf * lax.rsqrt(meansq + 1e-06) * mixer_gain).astype(jnp.bfloat16)
    gate = jnp.dot(normed, gate_weight, preferred_element_type=jnp.float32)
    up = jnp.dot(normed, up_weight, preferred_element_type=jnp.float32)
    hidden = (jax.nn.silu(gate) * up).astype(jnp.bfloat16)
    blocks = FF // N_TP
    hidden_blocks = hidden.reshape(TOKENS, N_TP, blocks).transpose(1, 0, 2)
    down_blocks = down_weight.reshape(N_TP, blocks, D)

    def add_block(total, pair):
        part = jnp.dot(pair[0], pair[1], preferred_element_type=jnp.float32).astype(jnp.bfloat16)
        part = lax.optimization_barrier(part)
        return (total + part.astype(jnp.float32), None)
    summed, unused = lax.scan(add_block, jnp.zeros((TOKENS, D), jnp.float32), (hidden_blocks, down_blocks))
    return (midf + summed).astype(jnp.bfloat16)
```

```python
import jax
import jax.numpy as jnp
from jax import lax
from jax.sharding import PartitionSpec as P

HD = 128
VD = 256
REACH = 4
SHARE = 4


def shifted(value, axis, by):
    length = lax.axis_size(axis)
    pairs = [(i, i + by) for i in range(length) if 0 <= i + by < length]
    return lax.ppermute(value, axis, pairs)


def groups(length):
    share = SHARE if length % SHARE == 0 else 1
    plane = [[i * share + j for j in range(share)] for i in range(length // share)]
    across = [[i * share + j for i in range(length // share)] for j in range(share)]
    return plane, across


def spread(blocks):
    length = lax.axis_size("sp")
    share = blocks.shape[0]
    if share == 1:
        return blocks
    mine = lax.rem(lax.axis_index("sp"), share)
    own = lax.dynamic_index_in_dim(blocks, mine, 0, keepdims=True)
    result = lax.dynamic_update_slice_in_dim(jnp.zeros_like(blocks), own, mine, 0)
    for by in range(1, share):
        pairs = [(i, i - i % share + (i + by) % share) for i in range(length)]
        sent = lax.dynamic_index_in_dim(blocks, lax.rem(mine + by, share), 0, keepdims=True)
        came = lax.ppermute(sent, "sp", pairs)
        result = lax.dynamic_update_slice_in_dim(result, came, lax.rem(mine + share - by, share), 0)
    return result


def gathered(gate_weight, up_weight, down_weight):
    plane, across = groups(lax.axis_size("sp"))
    share = len(plane[0])
    depth, units = gate_weight.shape
    part = units // share
    both = [gate_weight.reshape(depth, share, part), up_weight.reshape(depth, share, part)]
    both = jnp.concatenate(both, 2).transpose(1, 0, 2)
    both = spread(both).reshape(share * depth, 2 * part)
    down = spread(down_weight.reshape(share, part, depth))
    down = down.transpose(1, 0, 2).reshape(part, share * depth)
    both = lax.all_gather(both, "sp", axis=0, tiled=True, axis_index_groups=across)
    down = lax.all_gather(down, "sp", axis=1, tiled=True, axis_index_groups=across)
    return both, down


def body(
    resid,
    query_one,
    key_one,
    query_two,
    key_two,
    values,
    mix_lambda,
    segments,
    head_gain,
    out_weight,
    mixer_gain,
    gate_weight,
    up_weight,
    down_weight,
):
    rows = query_one.shape[0]
    heads = mix_lambda.shape[0]
    position = lax.axis_index("sp")
    both_all, down_all = gathered(gate_weight, up_weight, down_weight)
    carried = (key_one, key_two, values, segments)
    earlier = [carried]
    for step in range(REACH):
        carried = shifted((carried[0], carried[1], carried[2], carried[3]), "sp", 1)
        earlier.insert(0, carried)
    width = (REACH + 1) * rows
    k_first = jnp.concatenate([piece[0] for piece in earlier], 0).reshape(width, heads, HD)
    k_second = jnp.concatenate([piece[1] for piece in earlier], 0).reshape(width, heads, HD)
    vals = jnp.concatenate([piece[2] for piece in earlier], 0).reshape(width, heads, VD)
    seg_key = jnp.concatenate([piece[3] for piece in earlier], 0)
    q_pos = position * rows + jnp.arange(rows, dtype=jnp.int32)
    k_pos = (position - REACH) * rows + jnp.arange(width, dtype=jnp.int32)
    allowed = (
        (seg_key[None, :] == segments[:, None])
        & (k_pos[None, :] <= q_pos[:, None])
        & (k_pos[None, :] >= 0)
    )

    def weights(query, keys):
        score = jnp.einsum(
            "qhd,khd->hqk", query.reshape(rows, heads, HD), keys, preferred_element_type=jnp.float32
        ) * HD ** (-0.5)
        score = jnp.where(allowed[None], score, -jnp.inf)
        score = score - jnp.max(score, axis=-1, keepdims=True)
        expo = jnp.exp(score)
        return (expo / jnp.sum(expo, axis=-1, keepdims=True)).astype(jnp.bfloat16)

    out_first = jnp.einsum(
        "hqk,khe->qhe", weights(query_one, k_first), vals, preferred_element_type=jnp.float32
    )
    out_second = jnp.einsum(
        "hqk,khe->qhe", weights(query_two, k_second), vals, preferred_element_type=jnp.float32
    )
    head_out = out_first - mix_lambda[None, :, None] * out_second
    meansq = jnp.mean(head_out * head_out, axis=-1, keepdims=True)
    attn_rows = (
        (head_out * lax.rsqrt(meansq + 1e-05) * head_gain)
        .reshape(rows, heads * VD)
        .astype(jnp.bfloat16)
    )
    attn_rows, both_all, down_all = lax.optimization_barrier((attn_rows, both_all, down_all))
    projected = jnp.dot(
        lax.all_gather(attn_rows, "tp", axis=1, tiled=True),
        out_weight,
        preferred_element_type=jnp.float32,
    )
    mid = (resid.astype(jnp.float32) + projected).astype(jnp.bfloat16)
    midf = mid.astype(jnp.float32)
    squares = lax.psum(jnp.sum(midf * midf, axis=1), "tp")
    channels = mid.shape[1] * lax.axis_size("tp")
    normed = (midf * lax.rsqrt(squares / channels + 1e-06)[:, None] * mixer_gain).astype(
        jnp.bfloat16
    )
    plane, across = groups(lax.axis_size("sp"))
    share = len(plane[0])
    if share > 1:
        normed = lax.all_gather(normed, "sp", axis=0, tiled=True, axis_index_groups=plane)
    whole_rows = lax.all_gather(normed, "tp", axis=1, tiled=True)
    part = both_all.shape[1] // 2
    gate = jnp.dot(whole_rows, both_all[:, :part], preferred_element_type=jnp.float32)
    up = jnp.dot(whole_rows, both_all[:, part:], preferred_element_type=jnp.float32)
    hidden = (jax.nn.silu(gate) * up).astype(jnp.bfloat16)
    terms = jnp.dot(hidden, down_all, preferred_element_type=jnp.float32)
    summed = lax.psum_scatter(
        terms.astype(jnp.bfloat16), "tp", scatter_dimension=1, tiled=True
    )
    if share > 1:
        summed = lax.psum_scatter(
            summed, "sp", scatter_dimension=0, tiled=True, axis_index_groups=plane
        )
    return (midf + summed.astype(jnp.float32)).astype(jnp.bfloat16)


def solution(mesh):
    in_specs = (
        P("sp", "tp"),
        P("sp", "tp"),
        P("sp", "tp"),
        P("sp", "tp"),
        P("sp", "tp"),
        P("sp", "tp"),
        P("tp"),
        P("sp"),
        P(),
        P(None, "tp"),
        P("tp"),
        P("sp", "tp"),
        P("sp", "tp"),
        P("tp", "sp"),
    )
    out_specs = P("sp", "tp")
    return jax.shard_map(body, mesh=mesh, in_specs=in_specs, out_specs=out_specs, check_vma=False)
```

```python
import jax
import jax.numpy as jnp
from jax import lax
from jax.sharding import PartitionSpec as P

HD = 128
VD = 256
REACH = 4
SHARE = 2


def shifted(value, axis, by):
    length = lax.axis_size(axis)
    pairs = [(i, i + by) for i in range(length) if 0 <= i + by < length]
    return lax.ppermute(value, axis, pairs)


def groups(length):
    share = SHARE if length % SHARE == 0 else 1
    plane = [[i * share + j for j in range(share)] for i in range(length // share)]
    across = [[i * share + j for i in range(length // share)] for j in range(share)]
    return plane, across


def spread(blocks):
    length = lax.axis_size("sp")
    share = blocks.shape[0]
    if share == 1:
        return blocks
    mine = lax.rem(lax.axis_index("sp"), share)
    own = lax.dynamic_index_in_dim(blocks, mine, 0, keepdims=True)
    result = lax.dynamic_update_slice_in_dim(jnp.zeros_like(blocks), own, mine, 0)
    for by in range(1, share):
        pairs = [(i, i - i % share + (i + by) % share) for i in range(length)]
        sent = lax.dynamic_index_in_dim(blocks, lax.rem(mine + by, share), 0, keepdims=True)
        came = lax.ppermute(sent, "sp", pairs)
        result = lax.dynamic_update_slice_in_dim(result, came, lax.rem(mine + share - by, share), 0)
    return result


def gathered(gate_weight, up_weight, down_weight):
    plane, across = groups(lax.axis_size("sp"))
    share = len(plane[0])
    depth, units = gate_weight.shape
    part = units // share
    both = [gate_weight.reshape(depth, share, part), up_weight.reshape(depth, share, part)]
    both = jnp.concatenate(both, 2).transpose(1, 0, 2)
    both = spread(both).reshape(share * depth, 2 * part)
    down = spread(down_weight.reshape(share, part, depth))
    down = down.transpose(1, 0, 2).reshape(part, share * depth)
    both = lax.all_gather(both, "sp", axis=0, tiled=True, axis_index_groups=across)
    down = lax.all_gather(down, "sp", axis=1, tiled=True, axis_index_groups=across)
    return both, down


def body(
    resid,
    query_one,
    key_one,
    query_two,
    key_two,
    values,
    mix_lambda,
    segments,
    head_gain,
    out_weight,
    mixer_gain,
    gate_weight,
    up_weight,
    down_weight,
):
    rows = query_one.shape[0]
    heads = mix_lambda.shape[0]
    position = lax.axis_index("sp")
    both_all, down_all = gathered(gate_weight, up_weight, down_weight)
    carried = (key_one, key_two, values, segments)
    earlier = [carried]
    for step in range(REACH):
        carried = shifted((carried[0], carried[1], carried[2], carried[3]), "sp", 1)
        earlier.insert(0, carried)
    width = (REACH + 1) * rows
    k_first = jnp.concatenate([piece[0] for piece in earlier], 0).reshape(width, heads, HD)
    k_second = jnp.concatenate([piece[1] for piece in earlier], 0).reshape(width, heads, HD)
    vals = jnp.concatenate([piece[2] for piece in earlier], 0).reshape(width, heads, VD)
    seg_key = jnp.concatenate([piece[3] for piece in earlier], 0)
    q_pos = position * rows + jnp.arange(rows, dtype=jnp.int32)
    k_pos = (position - REACH) * rows + jnp.arange(width, dtype=jnp.int32)
    allowed = (
        (seg_key[None, :] == segments[:, None])
        & (k_pos[None, :] <= q_pos[:, None])
        & (k_pos[None, :] >= 0)
    )

    def weights(query, keys):
        score = jnp.einsum(
            "qhd,khd->hqk", query.reshape(rows, heads, HD), keys, preferred_element_type=jnp.float32
        ) * HD ** (-0.5)
        score = jnp.where(allowed[None], score, -jnp.inf)
        score = score - jnp.max(score, axis=-1, keepdims=True)
        expo = jnp.exp(score)
        return (expo / jnp.sum(expo, axis=-1, keepdims=True)).astype(jnp.bfloat16)

    out_first = jnp.einsum(
        "hqk,khe->qhe", weights(query_one, k_first), vals, preferred_element_type=jnp.float32
    )
    out_second = jnp.einsum(
        "hqk,khe->qhe", weights(query_two, k_second), vals, preferred_element_type=jnp.float32
    )
    head_out = out_first - mix_lambda[None, :, None] * out_second
    meansq = jnp.mean(head_out * head_out, axis=-1, keepdims=True)
    attn_rows = (
        (head_out * lax.rsqrt(meansq + 1e-05) * head_gain)
        .reshape(rows, heads * VD)
        .astype(jnp.bfloat16)
    )
    attn_rows, both_all, down_all = lax.optimization_barrier((attn_rows, both_all, down_all))
    projected = jnp.dot(
        lax.all_gather(attn_rows, "tp", axis=1, tiled=True),
        out_weight,
        preferred_element_type=jnp.float32,
    )
    mid = (resid.astype(jnp.float32) + projected).astype(jnp.bfloat16)
    midf = mid.astype(jnp.float32)
    squares = lax.psum(jnp.sum(midf * midf, axis=1), "tp")
    channels = mid.shape[1] * lax.axis_size("tp")
    normed = (midf * lax.rsqrt(squares / channels + 1e-06)[:, None] * mixer_gain).astype(
        jnp.bfloat16
    )
    plane, across = groups(lax.axis_size("sp"))
    share = len(plane[0])
    if share > 1:
        normed = lax.all_gather(normed, "sp", axis=0, tiled=True, axis_index_groups=plane)
    whole_rows = lax.all_gather(normed, "tp", axis=1, tiled=True)
    part = both_all.shape[1] // 2
    gate = jnp.dot(whole_rows, both_all[:, :part], preferred_element_type=jnp.float32)
    up = jnp.dot(whole_rows, both_all[:, part:], preferred_element_type=jnp.float32)
    hidden = (jax.nn.silu(gate) * up).astype(jnp.bfloat16)
    terms = jnp.dot(hidden, down_all, preferred_element_type=jnp.float32)
    summed = lax.psum_scatter(
        terms.astype(jnp.bfloat16), "tp", scatter_dimension=1, tiled=True
    )
    if share > 1:
        summed = lax.psum_scatter(
            summed, "sp", scatter_dimension=0, tiled=True, axis_index_groups=plane
        )
    return (midf + summed.astype(jnp.float32)).astype(jnp.bfloat16)


def solution(mesh):
    in_specs = (
        P("sp", "tp"),
        P("sp", "tp"),
        P("sp", "tp"),
        P("sp", "tp"),
        P("sp", "tp"),
        P("sp", "tp"),
        P("tp"),
        P("sp"),
        P(),
        P(None, "tp"),
        P("tp"),
        P("sp", "tp"),
        P("sp", "tp"),
        P("tp", "sp"),
    )
    out_specs = P("sp", "tp")
    return jax.shard_map(body, mesh=mesh, in_specs=in_specs, out_specs=out_specs, check_vma=False)
```

```python
import jax
import jax.numpy as jnp
from jax import lax
from jax.sharding import PartitionSpec as P

HD = 128
VD = 256
REACH = 4
SHARE = 2


def shifted(value, axis, by):
    length = lax.axis_size(axis)
    pairs = [(i, i + by) for i in range(length) if 0 <= i + by < length]
    return lax.ppermute(value, axis, pairs)


def groups(length):
    share = SHARE if length % SHARE == 0 else 1
    plane = [[i * share + j for j in range(share)] for i in range(length // share)]
    across = [[i * share + j for i in range(length // share)] for j in range(share)]
    return plane, across


def spread(blocks):
    length = lax.axis_size("sp")
    share = blocks.shape[0]
    if share == 1:
        return blocks
    mine = lax.rem(lax.axis_index("sp"), share)
    own = lax.dynamic_index_in_dim(blocks, mine, 0, keepdims=True)
    result = lax.dynamic_update_slice_in_dim(jnp.zeros_like(blocks), own, mine, 0)
    for by in range(1, share):
        pairs = [(i, i - i % share + (i + by) % share) for i in range(length)]
        sent = lax.dynamic_index_in_dim(blocks, lax.rem(mine + by, share), 0, keepdims=True)
        came = lax.ppermute(sent, "sp", pairs)
        result = lax.dynamic_update_slice_in_dim(result, came, lax.rem(mine + share - by, share), 0)
    return result


def gathered(gate_weight, up_weight, down_weight):
    plane, across = groups(lax.axis_size("sp"))
    share = len(plane[0])
    depth, units = gate_weight.shape
    part = units // share
    both = [gate_weight.reshape(depth, share, part), up_weight.reshape(depth, share, part)]
    both = jnp.concatenate(both, 2).transpose(1, 0, 2)
    both = spread(both).reshape(share * depth, 2 * part)
    down = spread(down_weight.reshape(share, part, depth))
    down = down.transpose(1, 0, 2).reshape(part, share * depth)
    both = lax.all_gather(both, "sp", axis=0, tiled=True, axis_index_groups=across)
    down = lax.all_gather(down, "sp", axis=1, tiled=True, axis_index_groups=across)
    return both, down


def swapped(value, axis, members):
    return lax.ppermute(value, axis, [(i, i ^ 1) for i in range(members)])


def whole_channels(value):
    members = lax.axis_size("tp")
    if members != 2:
        return lax.all_gather(value, "tp", axis=1, tiled=True)
    other = swapped(value, "tp", members)
    mine = lax.axis_index("tp") * value.shape[1]
    result = jnp.zeros((value.shape[0], 2 * value.shape[1]), value.dtype)
    result = lax.dynamic_update_slice_in_dim(result, value, mine, 1)
    return lax.dynamic_update_slice_in_dim(result, other, value.shape[1] - mine, 1)


def own_channels(terms):
    members = lax.axis_size("tp")
    if members != 2:
        return lax.psum_scatter(terms, "tp", scatter_dimension=1, tiled=True).astype(jnp.float32)
    width = terms.shape[1] // 2
    mine = lax.axis_index("tp") * width
    other = swapped(lax.dynamic_slice_in_dim(terms, width - mine, width, 1), "tp", members)
    own = lax.dynamic_slice_in_dim(terms, mine, width, 1)
    return own.astype(jnp.float32) + other.astype(jnp.float32)


def body(
    resid,
    query_one,
    key_one,
    query_two,
    key_two,
    values,
    mix_lambda,
    segments,
    head_gain,
    out_weight,
    mixer_gain,
    gate_weight,
    up_weight,
    down_weight,
):
    rows = query_one.shape[0]
    heads = mix_lambda.shape[0]
    position = lax.axis_index("sp")
    both_all, down_all = gathered(gate_weight, up_weight, down_weight)
    carried = (key_one, key_two, values, segments)
    earlier = [carried]
    for step in range(REACH):
        carried = shifted((carried[0], carried[1], carried[2], carried[3]), "sp", 1)
        earlier.insert(0, carried)
    width = (REACH + 1) * rows
    k_first = jnp.concatenate([piece[0] for piece in earlier], 0).reshape(width, heads, HD)
    k_second = jnp.concatenate([piece[1] for piece in earlier], 0).reshape(width, heads, HD)
    vals = jnp.concatenate([piece[2] for piece in earlier], 0).reshape(width, heads, VD)
    seg_key = jnp.concatenate([piece[3] for piece in earlier], 0)
    q_pos = position * rows + jnp.arange(rows, dtype=jnp.int32)
    k_pos = (position - REACH) * rows + jnp.arange(width, dtype=jnp.int32)
    allowed = (
        (seg_key[None, :] == segments[:, None])
        & (k_pos[None, :] <= q_pos[:, None])
        & (k_pos[None, :] >= 0)
    )

    def weights(query, keys):
        score = jnp.einsum(
            "qhd,khd->hqk", query.reshape(rows, heads, HD), keys, preferred_element_type=jnp.float32
        ) * HD ** (-0.5)
        score = jnp.where(allowed[None], score, -jnp.inf)
        score = score - jnp.max(score, axis=-1, keepdims=True)
        expo = jnp.exp(score)
        return (expo / jnp.sum(expo, axis=-1, keepdims=True)).astype(jnp.bfloat16)

    out_first = jnp.einsum(
        "hqk,khe->qhe", weights(query_one, k_first), vals, preferred_element_type=jnp.float32
    )
    out_second = jnp.einsum(
        "hqk,khe->qhe", weights(query_two, k_second), vals, preferred_element_type=jnp.float32
    )
    head_out = out_first - mix_lambda[None, :, None] * out_second
    meansq = jnp.mean(head_out * head_out, axis=-1, keepdims=True)
    attn_rows = (
        (head_out * lax.rsqrt(meansq + 1e-05) * head_gain)
        .reshape(rows, heads * VD)
        .astype(jnp.bfloat16)
    )
    projected = jnp.dot(
        whole_channels(attn_rows),
        out_weight,
        preferred_element_type=jnp.float32,
    )
    mid = (resid.astype(jnp.float32) + projected).astype(jnp.bfloat16)
    midf = mid.astype(jnp.float32)
    squares = lax.psum(jnp.sum(midf * midf, axis=1), "tp")
    channels = mid.shape[1] * lax.axis_size("tp")
    normed = (midf * lax.rsqrt(squares / channels + 1e-06)[:, None] * mixer_gain).astype(
        jnp.bfloat16
    )
    members = lax.axis_size("sp")
    paired = len(groups(members)[0][0]) == 2
    if paired:
        normed = jnp.concatenate([normed, swapped(normed, "sp", members)], 0)
    whole_rows = whole_channels(normed)
    whole_rows, both_all, down_all = lax.optimization_barrier((whole_rows, both_all, down_all))
    part = both_all.shape[1] // 2
    gate = jnp.dot(whole_rows, both_all[:, :part], preferred_element_type=jnp.float32)
    up = jnp.dot(whole_rows, both_all[:, part:], preferred_element_type=jnp.float32)
    hidden = (jax.nn.silu(gate) * up).astype(jnp.bfloat16)
    terms = jnp.dot(hidden, down_all, preferred_element_type=jnp.float32)
    summed = own_channels(terms.astype(jnp.bfloat16))
    if paired:
        came = swapped(summed[rows:].astype(jnp.bfloat16), "sp", members)
        summed = summed[:rows] + came.astype(jnp.float32)
    return (midf + summed).astype(jnp.bfloat16)


def solution(mesh):
    in_specs = (
        P("sp", "tp"),
        P("sp", "tp"),
        P("sp", "tp"),
        P("sp", "tp"),
        P("sp", "tp"),
        P("sp", "tp"),
        P("tp"),
        P("sp"),
        P(),
        P(None, "tp"),
        P("tp"),
        P("sp", "tp"),
        P("sp", "tp"),
        P("tp", "sp"),
    )
    out_specs = P("sp", "tp")
    return jax.shard_map(body, mesh=mesh, in_specs=in_specs, out_specs=out_specs, check_vma=False)
```
